32 devices in a mesh: grp: 2 (over y), kv: 4 (over z), tp: 4 (over x, core).
Axes of the slice: x: 2, y: 2, z: 4, core: 2. Of those that a mesh axis runs over, the one named last changes fastest.
Arguments:
- tokens: bfloat16 [160, 4096], P('grp', ('kv', 'tp')), parts along dimension 0, may hold values from -65 to 65
- lengths: int32 [160], P(('grp', 'kv')), parts along dimension 0, may hold values from 1 to 16384, 327680 in all
- memory: float32 [160, 16, 128, 128], P(('grp', 'kv'), 'tp'), parts along dimension 0, may hold values from -6 to 6
- norm_attn: bfloat16 [4096], P('kv'), may hold values from 0.099609375 to 1.8984375
- w_query: bfloat16 [4096, 2048], P('kv', 'tp'), may hold values from -0.09375 to 0.09375
- w_key: bfloat16 [4096, 2048], P('kv', 'tp'), may hold values from -0.09375 to 0.09375
- w_value: bfloat16 [4096, 2048], P('kv', 'tp'), may hold values from -0.09375 to 0.09375
- w_gate: bfloat16 [4096, 2048], P('kv', 'tp'), may hold values from -0.09375 to 0.09375
- head_gain: bfloat16 [2048], P('tp'), may hold values from 0.099609375 to 1.8984375
- w_out: bfloat16 [2048, 4096], P('tp', 'kv'), may hold values from -0.1875 to 0.1875
- norm_mlp: bfloat16 [4096], P('kv'), may hold values from 0.099609375 to 1.8984375
- w_gate_mlp: bfloat16 [4096, 14336], P('kv', 'tp'), may hold values from -0.09375 to 0.09375
- w_up: bfloat16 [4096, 14336], P('kv', 'tp'), may hold values from -0.09375 to 0.09375
- w_down: bfloat16 [14336, 4096], P('tp', 'kv'), may hold values from -0.0625 to 0.0625
Outputs:
- result: bfloat16 [160, 4096], P('grp', ('kv', 'tp')), parts along dimension 0
- new_memory: float32 [160, 16, 128, 128], P(('grp', 'kv'), 'tp'), parts along dimension 0
The draws below stay inside these ranges and needn't reach their ends.
There are 2 independent parts, one for each index of `grp`. The reference program is written for one: setup_inputs(seed, part) draws one part's arguments, and reference() takes and returns one part's arrays. A program takes and returns all parts, laid end to end along the dimension named above; an argument that names none is the same for every part. Nothing has to cross between parts.
Inputs may be any that keep to these rules, and one draw needn't show every extreme that they name: Within each part along grp the lengths sum to 327680 and the longest is exactly 16384.
All inputs are finite; a program needn't handle non-finite values. No bound on the sum of `lengths` on one device may be relied on, other than what follows from the above.
Results may differ from the reference program's by a relative error of at most 0.025.
Values may be sent and summed in bfloat16 or wider, within the bound.
A program may use at most 64 MiB of HBM per device.

```python
import math
import jax
import jax.numpy as jnp
import numpy as np
from jax import lax

D = 4096
HEADS = 16
HEAD = 128
FF = 14336
MAXLEN = 16384
BATCH = 80
RET_WIDTH = 2048


def draw_tokens(key, part):
    noise = jnp.clip(jax.random.normal(jax.random.fold_in(key, 1), (BATCH, D), jnp.float32), -6.0, 6.0)
    column = jnp.arange(D, dtype=jnp.float32) / D
    values = noise * (3.0 ** column)[None, :] * 0.6
    return values.astype(jnp.bfloat16)


def raised(array, stream_key, source, target, blocks, factor):
    def block_of(axis_at):
        return (jnp.arange(array.shape[axis_at]) // (array.shape[axis_at] // blocks)).reshape((-1,) + (1,) * (array.ndim - 1 - axis_at))

    one_side = jax.random.permutation(stream_key, blocks)[block_of(target)]
    far = (block_of(target) + blocks // 2) % blocks
    return jnp.where((block_of(source) == one_side) | (block_of(source) == far), factor * array, array)


def steps_of(own_key, shape, split, least, top_value):
    def one(axis_at, parts):
        draws = jax.random.uniform(jax.random.fold_in(jax.random.fold_in(own_key, 6), axis_at), (parts,), jnp.float32, least / len(split), top_value / len(split))
        return jnp.repeat(jnp.exp(draws), shape[axis_at] // parts).reshape((-1,) + (1,) * (len(shape) - axis_at - 1))

    gain = one(*split[0])
    for cut in split[1:]:
        gain = gain * one(*cut)
    return gain


def length_profile(number_of, total, most, lean):
    loads = [(1 << 20) // math.isqrt(rank ** lean) + 1 for rank in range(2, number_of + 1)]
    surplus, holding = total - most - (number_of - 1), [1] * (number_of - 1)
    while surplus > 0:
        candidates = [i for i in range(number_of - 1) if holding[i] < most]
        mass, budget = sum([loads[i] for i in candidates]), surplus
        for i in candidates:
            addition = min(most - holding[i], max(1, budget * loads[i] // mass), surplus)
            holding[i] = holding[i] + addition
            surplus = surplus - addition
    return np.array([most] + holding)


def ragged_sizes(stream_key, count, total, limit, slope):
    if count == 2:
        one = jax.random.randint(stream_key, (), max(1, total - limit), min(limit, total - 1) + 1)
        return jnp.stack([one, total - one])
    tallies = jnp.asarray(length_profile(count, total, limit, slope), jnp.int32)
    pairs = (count - 1) // 2
    donor, sink = tallies[1:1 + 2 * pairs:2], tallies[2:2 + 2 * pairs:2]
    slack = jnp.minimum(donor - 1, limit - sink)
    moved = jax.random.randint(jax.random.fold_in(stream_key, 1), (pairs,), 0, 1 << 20) % (slack + 1)
    tallies = tallies.at[1:1 + 2 * pairs:2].set(donor - moved).at[2:2 + 2 * pairs:2].set(sink + moved)
    return tallies[jax.random.permutation(jax.random.fold_in(stream_key, 2), count)]


def normal_values(own_key, extent, width, most, pieces=(), held_as=jnp.bfloat16):
    array = width * jax.random.normal(own_key, extent, jnp.float32)
    if pieces:
        array = array * steps_of(own_key, extent, pieces, -0.22, 0.18)
    return jnp.clip(array, -most, most).astype(held_as)


def noise_with(own_key, dims, deviation, limit, pieces, heavy, kind=jnp.bfloat16):
    values = deviation * jax.random.normal(own_key, dims, jnp.float32)
    if pieces:
        values = values * steps_of(own_key, dims, pieces, -0.22, 0.18)
    return jnp.clip(raised(values, jax.random.fold_in(own_key, 3), *heavy), -limit, limit).astype(kind)


def setup_inputs(seed: int = 0, part: int = 0) -> dict:
    arg_keys = jax.random.split(jax.random.key(seed), 15)
    own_keys = jax.random.split(jax.random.fold_in(arg_keys[14], part), 15)
    tokens = draw_tokens(jax.random.fold_in(jax.random.fold_in(arg_keys[14], part), 71), part)
    lengths = ragged_sizes(own_keys[1], BATCH, BATCH * MAXLEN // 4, MAXLEN, 2).astype(jnp.int32)
    memory = normal_values(own_keys[2], (BATCH, HEADS, HEAD, HEAD), 1.0, 6.0, ((0, 4), (1, 4)), jnp.float32)
    norm_attn = jnp.clip(1.0 + 0.18 * jax.random.normal(arg_keys[3], (D,), jnp.float32), 0.099609375, 1.8984375).astype(jnp.bfloat16)
    w_query = normal_values(arg_keys[4], (D, RET_WIDTH), D ** -0.5, 0.09375, ((0, 4), (1, 4)))
    w_key = normal_values(arg_keys[5], (D, RET_WIDTH), D ** -0.5, 0.09375, ((0, 4), (1, 4)))
    w_value = normal_values(arg_keys[6], (D, RET_WIDTH), D ** -0.5, 0.09375, ((0, 4), (1, 4)))
    w_gate = normal_values(arg_keys[7], (D, RET_WIDTH), D ** -0.5, 0.09375, ((0, 4), (1, 4)))
    head_gain = jnp.clip(1.0 + 0.18 * jax.random.normal(arg_keys[8], (RET_WIDTH,), jnp.float32), 0.099609375, 1.8984375).astype(jnp.bfloat16)
    w_out = noise_with(arg_keys[9], (RET_WIDTH, D), RET_WIDTH ** -0.5, 0.1875, ((0, 4), (1, 4)), (0, 1, 4, 2.0))
    norm_mlp = jnp.clip(1.0 + 0.18 * jax.random.normal(arg_keys[10], (D,), jnp.float32), 0.099609375, 1.8984375).astype(jnp.bfloat16)
    w_gate_mlp = normal_values(arg_keys[11], (D, FF), D ** -0.5, 0.09375, ((0, 4), (1, 4)))
    w_up = normal_values(arg_keys[12], (D, FF), D ** -0.5, 0.09375, ((0, 4), (1, 4)))
    w_down = noise_with(arg_keys[13], (FF, D), FF ** -0.5, 0.0625, ((0, 4), (1, 4)), (0, 1, 4, 2.0))
    return dict(tokens=tokens, lengths=lengths, memory=memory, norm_attn=norm_attn, w_query=w_query, w_key=w_key, w_value=w_value, w_gate=w_gate, head_gain=head_gain, w_out=w_out, norm_mlp=norm_mlp, w_gate_mlp=w_gate_mlp, w_up=w_up, w_down=w_down)


epsilon = 1e-06

def rotate(values, position):
    half_width = values.shape[-1] // 2
    inverse = 10000.0 ** (-jnp.arange(half_width, dtype=jnp.float32) / half_width)
    angles = position[:, None] * inverse[None, :]
    cosine = jnp.cos(angles)[:, None, :]
    sine = jnp.sin(angles)[:, None, :]
    first = values[..., :half_width]
    second = values[..., half_width:]
    return jnp.concatenate([first * cosine - second * sine, second * cosine + first * sine], axis=-1)

def head_decay(head_index):
    exponent = -5.0 - head_index.astype(jnp.float32) * (7.0 / max(HEADS - 1, 1))
    return 1.0 - jnp.exp2(exponent)

def retain(memory, queries, key_rows, value_rows, gate_rows, head_gain, decay_rate):
    new_memory = decay_rate[None, :, None, None] * memory + key_rows[:, :, :, None] * value_rows[:, :, None, :]
    readout = jnp.einsum('bhd,bhde->bhe', queries * queries.shape[-1] ** (-0.5), new_memory, precision=lax.Precision.HIGHEST)
    centred = readout - lax.optimization_barrier(jnp.mean(readout, axis=-1, keepdims=True))
    normed = centred * lax.rsqrt(lax.optimization_barrier(jnp.mean(centred * centred, axis=-1, keepdims=True)) + epsilon)
    normed = normed.reshape(readout.shape[0], -1) * head_gain.astype(jnp.float32)
    return (new_memory, (normed * jax.nn.silu(gate_rows)).astype(jnp.bfloat16))

def reference(tokens, lengths, memory, norm_attn, w_query, w_key, w_value, w_gate, head_gain, w_out, norm_mlp, w_gate_mlp, w_up, w_down):
    tok_float = tokens.astype(jnp.float32)
    inv_attn = lax.rsqrt(lax.optimization_barrier(jnp.sum(tok_float * tok_float, axis=1)) / D + epsilon)
    scaled = (tok_float * norm_attn.astype(jnp.float32)).astype(jnp.bfloat16)

    def project(weight):
        return inv_attn[:, None] * jnp.dot(scaled, weight, preferred_element_type=jnp.float32)
    position = lengths.astype(jnp.float32)
    batch_rows = tokens.shape[0]
    queries = rotate(project(w_query).reshape(batch_rows, HEADS, HEAD), position)
    key_rows = rotate(project(w_key).reshape(batch_rows, HEADS, HEAD), position)
    value_rows = project(w_value).reshape(batch_rows, HEADS, HEAD)
    gate_rows = project(w_gate)
    decay_rate = head_decay(jnp.arange(HEADS))
    new_memory, mixed = retain(memory, queries, key_rows, value_rows, gate_rows, head_gain, decay_rate)
    middle = (tok_float + jnp.dot(mixed, w_out, preferred_element_type=jnp.float32)).astype(jnp.bfloat16)
    mid_float = middle.astype(jnp.float32)
    inv_mlp = lax.rsqrt(lax.optimization_barrier(jnp.sum(mid_float * mid_float, axis=1)) / D + epsilon)
    scaled_mid = (mid_float * norm_mlp.astype(jnp.float32)).astype(jnp.bfloat16)
    gate_mlp = inv_mlp[:, None] * jnp.dot(scaled_mid, w_gate_mlp, preferred_element_type=jnp.float32)
    up_rows = inv_mlp[:, None] * jnp.dot(scaled_mid, w_up, preferred_element_type=jnp.float32)
    hidden = (jax.nn.silu(gate_mlp) * up_rows).astype(jnp.bfloat16)
    result = (mid_float + jnp.dot(hidden, w_down, preferred_element_type=jnp.float32)).astype(jnp.bfloat16)
    return (result, new_memory)
```

```python
import functools

import jax
import jax.numpy as jnp
from jax import lax
from jax.experimental import pallas as pl
from jax.experimental.pallas import tpu as pltpu
from jax.sharding import PartitionSpec as P

HEADS = 16
EPS = 1e-06
F32 = jnp.float32
BF16 = jnp.bfloat16
MESH = pl.DeviceIdType.MESH


def head_decay(head_index):
    exponent = -5.0 - head_index.astype(F32) * (7.0 / max(HEADS - 1, 1))
    return 1.0 - jnp.exp2(exponent)


def dot(a, b):
    return jnp.dot(a, b, preferred_element_type=F32)


def chunk_width(ff_local):
    return 512 if ff_local % 512 == 0 else 128


def start_all(axis, n, me, src_of, dst, ssem, rsem):
    copies = []
    for d in range(1, n):
        other = lax.rem(me + d, n)
        copy = pltpu.make_async_remote_copy(
            src_ref=src_of(other),
            dst_ref=dst.at[me],
            send_sem=ssem.at[d - 1],
            recv_sem=rsem.at[me],
            device_id={axis: other},
            device_id_type=MESH,
        )
        copy.start()
        copies.append(copy)
    return copies


def wait_all(axis, n, me, dst, ssem, rsem):
    for d in range(1, n):
        other = lax.rem(me + d, n)
        pltpu.make_async_remote_copy(
            src_ref=dst.at[other],
            dst_ref=dst.at[other],
            send_sem=ssem.at[d - 1],
            recv_sem=rsem.at[other],
            device_id={axis: other},
            device_id_type=MESH,
        ).wait_recv()


def spread(width, total, start):
    rows = lax.broadcasted_iota(jnp.int32, (width, total), 0)
    cols = lax.broadcasted_iota(jnp.int32, (width, total), 1)
    return jnp.where(rows + start == cols, 1.0, 0.0).astype(BF16)


def pick(width, total, start):
    rows = lax.broadcasted_iota(jnp.int32, (total, width), 0)
    cols = lax.broadcasted_iota(jnp.int32, (total, width), 1)
    return jnp.where(rows == cols + start, 1.0, 0.0).astype(BF16)


def joined(blocks, dt, tp):
    if dt % 128 == 0:
        return jnp.concatenate([blocks[j].astype(F32) for j in range(tp)], axis=1)
    total = dot(blocks[0], spread(dt, dt * tp, 0))
    for j in range(1, tp):
        total = total + dot(blocks[j], spread(dt, dt * tp, j * dt))
    return total


def cut(part, buffer, dt, tp):
    if dt % 128 == 0:
        for j in range(tp):
            buffer[j] = part[:, j * dt : (j + 1) * dt].astype(BF16)
    else:
        whole = part.astype(BF16)
        for j in range(tp):
            buffer[j] = dot(whole, pick(dt, dt * tp, j * dt)).astype(BF16)


def kernel(
    kv, tp, model_width,
    tokens, cosine, sine, norm_attn, norm_mlp, gain,
    memory_h, wq_h, wk_h, wv_h, wg_h, wo_h, wgm_h, wup_h, wd_h,
    result, k_out, v_out,
    memory, wq, wk, wv, wg, wo, wgm, wup, wd,
    tok_all, p32, psend, precv, sq_send, sq_recv, qpad, ro, mixed_all, m32,
    asend, arecv, mid_all, msq_send, msq_recv, f32buf, fsend, frecv, h_all, acc, dsend, drecv,
    lsem, tok_s, tok_r, sq_s, sq_r, p_s, p_r, mx_s, mx_r, a_s, a_r, md_s, md_r, ms_s, ms_r,
    f_s, f_r, h_s, h_r, d_s, d_r,
):
    z = lax.axis_index("kv")
    t = lax.axis_index("tp")
    rows, dt = tokens.shape
    own, heads, head, _ = memory.shape
    wl = heads * head
    ff = wup.shape[1]
    cw = chunk_width(ff)
    chunks = ff // cw

    local = []
    for i, (src, dst) in enumerate(
        [(wq_h, wq), (wk_h, wk), (wv_h, wv), (wg_h, wg), (memory_h, memory),
         (wo_h, wo), (wgm_h, wgm), (wup_h, wup), (wd_h, wd)]
    ):
        copy = pltpu.make_async_copy(src, dst, lsem.at[i])
        copy.start()
        local.append(copy)

    barrier = pltpu.get_barrier_semaphore()
    for d in range(1, kv):
        pl.semaphore_signal(barrier, inc=1, device_id={"kv": lax.rem(z + d, kv)}, device_id_type=MESH)
    for d in range(1, tp):
        pl.semaphore_signal(barrier, inc=1, device_id={"tp": lax.rem(t + d, tp)}, device_id_type=MESH)
    pl.semaphore_wait(barrier, kv + tp - 2)

    sends = []
    sends += start_all("tp", tp, t, lambda k: tokens, tok_all, tok_s, tok_r)
    tok_all[t] = tokens[...]
    wait_all("tp", tp, t, tok_all, tok_s, tok_r)
    tok = joined(tok_all, dt, tp)
    scaled = (tok * norm_attn[...]).astype(BF16)
    m32[:, 0:128] = jnp.broadcast_to(jnp.sum(tok * tok, axis=1, keepdims=True), (rows, 128))
    for k in range(kv):
        sq_send[k] = m32[k * own : (k + 1) * own, 0:128]
    sends += start_all("kv", kv, z, lambda k: sq_send.at[k], sq_recv, sq_s, sq_r)
    sq_recv[z] = sq_send[z]

    for i, w in enumerate((wq, wk, wv, wg)):
        local[i].wait()
        p32[:, i * wl : (i + 1) * wl] = dot(scaled, w[...])
    for k in range(kv):
        psend[k] = p32[k * own : (k + 1) * own, :].astype(BF16)
    sends += start_all("kv", kv, z, lambda k: psend.at[k], precv, p_s, p_r)
    precv[z] = psend[z]
    qpad[...] = jnp.zeros(qpad.shape, F32)
    wait_all("kv", kv, z, sq_recv, sq_s, sq_r)
    squares = sq_recv[0]
    for k in range(1, kv):
        squares = squares + sq_recv[k]
    inv = lax.rsqrt(squares / model_width + EPS)
    local[4].wait()
    wait_all("kv", kv, z, precv, p_s, p_r)

    def column(start):
        total = precv[0, :, start : start + head].astype(F32)
        for k in range(1, kv):
            total = total + precv[k, :, start : start + head].astype(F32)
        return total * inv

    cos = cosine[...]
    sin = sine[...]
    for h in range(heads):
        q = column(h * head)
        q = (q * cos + pltpu.roll(q, head // 2, 1) * sin) * head ** (-0.5)
        kk = column(wl + h * head)
        kk = kk * cos + pltpu.roll(kk, head // 2, 1) * sin
        v = column(2 * wl + h * head)
        g = column(3 * wl + h * head)
        k_out[:, h * head : (h + 1) * head] = kk
        v_out[:, h * head : (h + 1) * head] = v
        qpad[0:own, :] = q
        q_t = jnp.transpose(qpad[...])
        for b in range(own):
            ro[b : b + 1, :] = jnp.sum(memory[b, h] * q_t[:, b : b + 1], axis=0, keepdims=True)
        exponent = -5.0 - (t * heads + h).astype(F32) * (7.0 / max(HEADS - 1, 1))
        decay = 1.0 - jnp.exp2(jnp.full((1, head), exponent, F32))
        readout = decay * ro[...] + jnp.sum(q * kk, axis=1, keepdims=True) * v
        centred = readout - jnp.mean(readout, axis=1, keepdims=True)
        normed = centred * lax.rsqrt(jnp.mean(centred * centred, axis=1, keepdims=True) + EPS)
        mixed = normed * gain[:, h * head : (h + 1) * head] * (g / (1.0 + jnp.exp(-g)))
        mixed_all[z, :, h * head : (h + 1) * head] = mixed.astype(BF16)

    sends += start_all("kv", kv, z, lambda k: mixed_all.at[z], mixed_all, mx_s, mx_r)
    local[5].wait()
    wait_all("kv", kv, z, mixed_all, mx_s, mx_r)
    for k in range(kv):
        m32[k * own : (k + 1) * own, :] = mixed_all[k].astype(F32)
    cut(dot(m32[...].astype(BF16), wo[...]), asend, dt, tp)
    sends += start_all("tp", tp, t, lambda k: asend.at[k], arecv, a_s, a_r)
    arecv[t] = asend[t]
    wait_all("tp", tp, t, arecv, a_s, a_r)
    total = arecv[0].astype(F32)
    for j in range(1, tp):
        total = total + arecv[j].astype(F32)
    mid_all[t] = (tokens[...].astype(F32) + total).astype(BF16)
    sends += start_all("tp", tp, t, lambda k: mid_all.at[t], mid_all, md_s, md_r)
    local[6].wait()
    local[7].wait()
    wait_all("tp", tp, t, mid_all, md_s, md_r)
    mid = joined(mid_all, dt, tp)
    scaled = (mid * norm_mlp[...]).astype(BF16)
    m32[:, 0:128] = jnp.broadcast_to(jnp.sum(mid * mid, axis=1, keepdims=True), (rows, 128))
    for k in range(kv):
        msq_send[k] = m32[k * own : (k + 1) * own, 0:128]
    sends += start_all("kv", kv, z, lambda k: msq_send.at[k], msq_recv, ms_s, ms_r)
    msq_recv[z] = msq_send[z]

    for c in range(chunks):
        f32buf[:, 0:cw] = dot(scaled, wgm[:, c * cw : (c + 1) * cw])
        f32buf[:, cw : 2 * cw] = dot(scaled, wup[:, c * cw : (c + 1) * cw])
        for k in range(kv):
            fsend[c, k] = f32buf[k * own : (k + 1) * own, :].astype(BF16)
        sends += start_all("kv", kv, z, lambda k: fsend.at[c, k], frecv.at[c], f_s.at[c], f_r.at[c])
        frecv[c, z] = fsend[c, z]

    wait_all("kv", kv, z, msq_recv, ms_s, ms_r)
    squares = msq_recv[0]
    for k in range(1, kv):
        squares = squares + msq_recv[k]
    inv = lax.rsqrt(squares / model_width + EPS)[:, 0:1]
    for c in range(chunks):
        wait_all("kv", kv, z, frecv.at[c], f_s.at[c], f_r.at[c])
        both = frecv[c, 0].astype(F32)
        for k in range(1, kv):
            both = both + frecv[c, k].astype(F32)
        both = both * inv
        g = both[:, 0:cw]
        h_all[c, z] = (g / (1.0 + jnp.exp(-g)) * both[:, cw : 2 * cw]).astype(BF16)
        sends += start_all("kv", kv, z, lambda k: h_all.at[c, z], h_all.at[c], h_s.at[c], h_r.at[c])
    local[8].wait()
    for c in range(chunks):
        wait_all("kv", kv, z, h_all.at[c], h_s.at[c], h_r.at[c])
        for k in range(kv):
            f32buf[k * own : (k + 1) * own, 0:cw] = h_all[c, k].astype(F32)
        part = dot(f32buf[:, 0:cw].astype(BF16), wd[c * cw : (c + 1) * cw, :])
        acc[...] = part if c == 0 else acc[...] + part
    cut(acc[...], dsend, dt, tp)
    sends += start_all("tp", tp, t, lambda k: dsend.at[k], drecv, d_s, d_r)
    drecv[t] = dsend[t]
    wait_all("tp", tp, t, drecv, d_s, d_r)
    total = drecv[0].astype(F32)
    for j in range(1, tp):
        total = total + drecv[j].astype(F32)
    result[...] = (mid_all[t].astype(F32) + total).astype(BF16)
    for copy in sends:
        copy.wait_send()


def per_device(kv, tp, tokens, lengths, memory, norm_attn, w_query, w_key, w_value, w_gate,
               head_gain, w_out, norm_mlp, w_gate_mlp, w_up, w_down):
    own, heads, head, _ = memory.shape
    rows, dt = tokens.shape
    dk, wl = w_query.shape
    ff = w_up.shape[1]
    cw = chunk_width(ff)
    chunks = ff // cw
    half = head // 2
    inverse = 10000.0 ** (-jnp.arange(half, dtype=F32) / half)
    inverse = jnp.concatenate([inverse, inverse])
    angles = lengths.astype(F32)[:, None] * inverse[None, :]
    sign = jnp.where(jnp.arange(head) < half, -1.0, 1.0)[None, :]
    vm = pl.BlockSpec(memory_space=pltpu.VMEM)
    hbm = pl.BlockSpec(memory_space=pl.ANY)
    dma = pltpu.SemaphoreType.DMA
    padded = -(-own // 8) * 8

    def pair(n, *lead):
        return [dma(lead + (n - 1,)), dma(lead + (n,))]

    scratch = [
        pltpu.VMEM(memory.shape, F32),
        *[pltpu.VMEM((dk, wl), BF16)] * 4,
        pltpu.VMEM((wl, dk), BF16),
        pltpu.VMEM((dk, ff), BF16),
        pltpu.VMEM((dk, ff), BF16),
        pltpu.VMEM((ff, dk), BF16),
        pltpu.VMEM((tp, rows, dt), BF16),
        pltpu.VMEM((rows, 4 * wl), F32),
        pltpu.VMEM((kv, own, 4 * wl), BF16),
        pltpu.VMEM((kv, own, 4 * wl), BF16),
        pltpu.VMEM((kv, own, 128), F32),
        pltpu.VMEM((kv, own, 128), F32),
        pltpu.VMEM((padded, head), F32),
        pltpu.VMEM((own, head), F32),
        pltpu.VMEM((kv, own, wl), BF16),
        pltpu.VMEM((rows, wl), F32),
        pltpu.VMEM((tp, rows, dt), BF16),
        pltpu.VMEM((tp, rows, dt), BF16),
        pltpu.VMEM((tp, rows, dt), BF16),
        pltpu.VMEM((kv, own, 128), F32),
        pltpu.VMEM((kv, own, 128), F32),
        pltpu.VMEM((rows, 2 * cw), F32),
        pltpu.VMEM((chunks, kv, own, 2 * cw), BF16),
        pltpu.VMEM((chunks, kv, own, 2 * cw), BF16),
        pltpu.VMEM((chunks, kv, own, cw), BF16),
        pltpu.VMEM((rows, dk), F32),
        pltpu.VMEM((tp, rows, dt), BF16),
        pltpu.VMEM((tp, rows, dt), BF16),
        dma((9,)),
        *pair(tp), *pair(kv), *pair(kv), *pair(kv), *pair(tp), *pair(tp), *pair(kv),
        *pair(kv, chunks), *pair(kv, chunks), *pair(tp),
    ]
    result, keys, values = pl.pallas_call(
        functools.partial(kernel, kv, tp, float(dk * kv)),
        out_shape=(
            jax.ShapeDtypeStruct((rows, dt), BF16),
            jax.ShapeDtypeStruct((own, wl), F32),
            jax.ShapeDtypeStruct((own, wl), F32),
        ),
        in_specs=[vm] * 6 + [hbm] * 9,
        out_specs=(vm, vm, vm),
        scratch_shapes=scratch,
        compiler_params=pltpu.CompilerParams(
            collective_id=0, has_side_effects=True, vmem_limit_bytes=60 * 1024 * 1024
        ),
    )(
        tokens, jnp.cos(angles), jnp.sin(angles) * sign,
        norm_attn.astype(F32)[None, :], norm_mlp.astype(F32)[None, :], head_gain.astype(F32)[None, :],
        memory, w_query, w_key, w_value, w_gate, w_out, w_gate_mlp, w_up, w_down,
    )
    decay = head_decay(lax.axis_index("tp") * heads + jnp.arange(heads))
    keys = keys.reshape(own, heads, head)
    values = values.reshape(own, heads, head)
    new_memory = (
        decay[None, :, None, None] * memory + keys[:, :, :, None] * values[:, :, None, :]
    )
    return result, new_memory


def solution(mesh):
    in_specs = (
        P("grp", ("kv", "tp")),
        P(("grp", "kv")),
        P(("grp", "kv"), "tp", None, None),
        P("kv"),
        P("kv", "tp"),
        P("kv", "tp"),
        P("kv", "tp"),
        P("kv", "tp"),
        P("tp"),
        P("tp", "kv"),
        P("kv"),
        P("kv", "tp"),
        P("kv", "tp"),
        P("tp", "kv"),
    )
    out_specs = (P("grp", ("kv", "tp")), P(("grp", "kv"), "tp", None, None))
    return jax.shard_map(
        functools.partial(per_device, mesh.shape["kv"], mesh.shape["tp"]),
        mesh=mesh, in_specs=in_specs, out_specs=out_specs, check_vma=False,
    )
```

```python
import functools

import jax
import jax.numpy as jnp
from jax import lax
from jax.experimental import pallas as pl
from jax.experimental.pallas import tpu as pltpu
from jax.sharding import PartitionSpec as P

HEADS = 16
EPS = 1e-06
F32 = jnp.float32
BF16 = jnp.bfloat16
MESH = pl.DeviceIdType.MESH


def dot(a, b):
    return jnp.dot(a, b, preferred_element_type=F32)


def chunk_width(ff_local):
    return 256 if ff_local % 256 == 0 else 128


SKEW = 2


def as_row(ref):
    parts = ref[...].astype(F32)
    return jnp.concatenate([parts[i : i + 1] for i in range(parts.shape[0])], axis=1)


def start_all(axis, n, me, src_of, dst, ssem, rsem):
    copies = []
    for d in range(1, n):
        other = lax.rem(me + d, n)
        copy = pltpu.make_async_remote_copy(
            src_ref=src_of(other),
            dst_ref=dst.at[me],
            send_sem=ssem.at[d - 1],
            recv_sem=rsem.at[me],
            device_id={axis: other},
            device_id_type=MESH,
        )
        copy.start()
        copies.append(copy)
    return copies


def wait_all(axis, n, me, dst, ssem, rsem):
    for d in range(1, n):
        other = lax.rem(me + d, n)
        pltpu.make_async_remote_copy(
            src_ref=dst.at[other],
            dst_ref=dst.at[other],
            send_sem=ssem.at[d - 1],
            recv_sem=rsem.at[other],
            device_id={axis: other},
            device_id_type=MESH,
        ).wait_recv()


def spread(width, total, start):
    rows = lax.broadcasted_iota(jnp.int32, (width, total), 0)
    cols = lax.broadcasted_iota(jnp.int32, (width, total), 1)
    return jnp.where(rows + start == cols, 1.0, 0.0).astype(BF16)


def pick(width, total, start):
    rows = lax.broadcasted_iota(jnp.int32, (total, width), 0)
    cols = lax.broadcasted_iota(jnp.int32, (total, width), 1)
    return jnp.where(rows == cols + start, 1.0, 0.0).astype(BF16)


def joined(blocks, dt, tp):
    if dt % 128 == 0:
        return jnp.concatenate([blocks[j].astype(F32) for j in range(tp)], axis=1)
    total = dot(blocks[0], spread(dt, dt * tp, 0))
    for j in range(1, tp):
        total = total + dot(blocks[j], spread(dt, dt * tp, j * dt))
    return total


def cut(part, buffer, dt, tp):
    if dt % 128 == 0:
        for j in range(tp):
            buffer[j] = part[:, j * dt : (j + 1) * dt].astype(BF16)
    else:
        whole = part.astype(BF16)
        for j in range(tp):
            buffer[j] = dot(whole, pick(dt, dt * tp, j * dt)).astype(BF16)


def kernel(
    kv, tp, model_width,
    tokens, cosine, sine, norm_attn, norm_mlp, gain_h,
    memory_h, wq_h, wk_h, wv_h, wg_h, wo_h, wgm_h, wup_h, wd_h,
    result, k_out, v_out,
    memory, wq, wk, wv, wg, wo, wgm, wup, wd,
    tok_all, p32, psend, precv, sq_send, sq_recv, qpad, qrot, ro, mixed_all, m32,
    asend, arecv, mid_all, msq_send, msq_recv, inv_ref, scaled_ref,
    part, csend, crecv, h_all, acc, dsend, drecv,
    lsem, tok_s, tok_r, sq_s, sq_r, p_s, p_r, mx_s, mx_r, a_s, a_r, md_s, md_r, d_s, d_r,
    ms_s, ms_r, c_s, c_r, h_s, h_r,
):
    z = lax.axis_index("kv")
    t = lax.axis_index("tp")
    rows, dt = tokens.shape
    own, heads, head, _ = memory.shape
    wl = heads * head
    ff = wup.shape[1]
    cw = chunk_width(ff)
    chunks = ff // cw

    local = []
    for i, (src, dst) in enumerate(
        [(wq_h, wq), (wk_h, wk), (wv_h, wv), (wg_h, wg), (memory_h, memory),
         (wo_h, wo), (wgm_h, wgm), (wup_h, wup), (wd_h, wd)]
    ):
        copy = pltpu.make_async_copy(src, dst, lsem.at[i])
        copy.start()
        local.append(copy)

    barrier = pltpu.get_barrier_semaphore()
    for d in range(1, kv):
        pl.semaphore_signal(barrier, inc=1, device_id={"kv": lax.rem(z + d, kv)}, device_id_type=MESH)
    for d in range(1, tp):
        pl.semaphore_signal(barrier, inc=1, device_id={"tp": lax.rem(t + d, tp)}, device_id_type=MESH)
    pl.semaphore_wait(barrier, kv + tp - 2)

    sends = []
    sends += start_all("tp", tp, t, lambda k: tokens, tok_all, tok_s, tok_r)
    tok_all[t] = tokens[...]
    wait_all("tp", tp, t, tok_all, tok_s, tok_r)
    tok = joined(tok_all, dt, tp)
    scaled = (tok * as_row(norm_attn)).astype(BF16)
    m32[:, 0:128] = jnp.broadcast_to(jnp.sum(tok * tok, axis=1, keepdims=True), (rows, 128))
    for k in range(kv):
        sq_send[k] = m32[k * own : (k + 1) * own, 0:128]
    sends += start_all("kv", kv, z, lambda k: sq_send.at[k], sq_recv, sq_s, sq_r)
    sq_recv[z] = sq_send[z]

    for i, w in enumerate((wq, wk, wv, wg)):
        local[i].wait()
        p32[...] = dot(scaled, w[...])
        for k in range(kv):
            psend[i, k] = p32[k * own : (k + 1) * own, :].astype(BF16)
        sends += start_all("kv", kv, z, lambda k: psend.at[i, k], precv.at[i], p_s.at[i], p_r.at[i])
        precv[i, z] = psend[i, z]
    qpad[...] = jnp.zeros(qpad.shape, F32)
    wait_all("kv", kv, z, sq_recv, sq_s, sq_r)
    squares = sq_recv[0]
    for k in range(1, kv):
        squares = squares + sq_recv[k]
    inv = lax.rsqrt(squares / model_width + EPS)

    def column(i, h):
        start = h * head
        total = precv[i, 0, :, start : start + head].astype(F32)
        for k in range(1, kv):
            total = total + precv[i, k, :, start : start + head].astype(F32)
        return total * inv

    cos = cosine[...]
    sin = sine[...]
    gain = as_row(gain_h)
    local[4].wait()
    wait_all("kv", kv, z, precv.at[0], p_s.at[0], p_r.at[0])
    for h in range(heads):
        q = column(0, h)
        q = (q * cos + pltpu.roll(q, head // 2, 1) * sin) * head ** (-0.5)
        qrot[h] = q
        qpad[h, 0:own, :] = q
        q_t = jnp.transpose(qpad[h])
        for b in range(own):
            ro[h, b : b + 1, :] = jnp.sum(memory[b, h] * q_t[:, b : b + 1], axis=0, keepdims=True)
    for i in (1, 2, 3):
        wait_all("kv", kv, z, precv.at[i], p_s.at[i], p_r.at[i])
    for h in range(heads):
        kk = column(1, h)
        kk = kk * cos + pltpu.roll(kk, head // 2, 1) * sin
        v = column(2, h)
        g = column(3, h)
        qpad[h, 0:own, :] = kk
        v_out[:, h * head : (h + 1) * head] = v
        exponent = -5.0 - (t * heads + h).astype(F32) * (7.0 / max(HEADS - 1, 1))
        decay = 1.0 - jnp.exp2(jnp.full((1, head), exponent, F32))
        readout = decay * ro[h] + jnp.sum(qrot[h] * kk, axis=1, keepdims=True) * v
        centred = readout - jnp.mean(readout, axis=1, keepdims=True)
        normed = centred * lax.rsqrt(jnp.mean(centred * centred, axis=1, keepdims=True) + EPS)
        mixed = normed * gain[:, h * head : (h + 1) * head] * (g / (1.0 + jnp.exp(-g)))
        mixed_all[z, :, h * head : (h + 1) * head] = mixed.astype(BF16)

    sends += start_all("kv", kv, z, lambda k: mixed_all.at[z], mixed_all, mx_s, mx_r)
    for h in range(heads):
        k_out[h] = jnp.transpose(qpad[h])
    local[5].wait()
    wait_all("kv", kv, z, mixed_all, mx_s, mx_r)
    for k in range(kv):
        m32[k * own : (k + 1) * own, :] = mixed_all[k].astype(F32)
    cut(dot(m32[...].astype(BF16), wo[...]), asend, dt, tp)
    sends += start_all("tp", tp, t, lambda k: asend.at[k], arecv, a_s, a_r)
    arecv[t] = asend[t]
    wait_all("tp", tp, t, arecv, a_s, a_r)
    total = arecv[0].astype(F32)
    for j in range(1, tp):
        total = total + arecv[j].astype(F32)
    mid_all[t] = (tokens[...].astype(F32) + total).astype(BF16)
    sends += start_all("tp", tp, t, lambda k: mid_all.at[t], mid_all, md_s, md_r)
    local[6].wait()
    local[7].wait()
    wait_all("tp", tp, t, mid_all, md_s, md_r)
    mid = joined(mid_all, dt, tp)
    scaled = (mid * as_row(norm_mlp)).astype(BF16)
    scaled_ref[...] = scaled
    mid_squares = jnp.broadcast_to(jnp.sum(mid * mid, axis=1, keepdims=True), (rows, 128))
    half = rows // 2
    last = kv - 1
    places = (z == 0, z == last)
    ends = (0, last)
    for side in (0, 1):
        msq_send[side] = mid_squares[side * half : (side + 1) * half]

    def squares_copy(side, sender):
        return pltpu.make_async_remote_copy(
            src_ref=msq_send.at[side],
            dst_ref=msq_recv.at[sender],
            send_sem=ms_s.at[side],
            recv_sem=ms_r.at[sender],
            device_id={"kv": ends[side]},
            device_id_type=MESH,
        )

    for side in (0, 1):
        @pl.when(jnp.logical_not(places[side]))
        def _():
            squares_copy(side, z).start()

    onward = (lax.rem(z + last, kv), lax.rem(z + 1, kv))
    depth = (last - z, z)

    def chain_copy(side, c):
        return pltpu.make_async_remote_copy(
            src_ref=csend.at[side, c],
            dst_ref=crecv.at[side, c],
            send_sem=c_s.at[side, c],
            recv_sem=c_r.at[side, c],
            device_id={"kv": onward[side]},
            device_id_type=MESH,
        )

    def hidden_copy(side, c):
        return pltpu.make_async_remote_copy(
            src_ref=h_all.at[side, c],
            dst_ref=h_all.at[side, c],
            send_sem=h_s.at[side, c],
            recv_sem=h_r.at[side, c],
            device_id={"kv": onward[1 - side]},
            device_id_type=MESH,
        )

    def within(c):
        return jnp.logical_and(c >= 0, c < chunks)

    acc[...] = jnp.zeros(acc.shape, F32)
    local[8].wait()
    full = SKEW * last

    def step(s, carry):
        @pl.when(s < chunks)
        def _():
            cols = pl.ds(pl.multiple_of(s * cw, cw), cw)
            lhs = scaled_ref[...]
            g = dot(lhs, wgm[:, cols])
            u = dot(lhs, wup[:, cols])
            for side in (0, 1):
                part[s, side, :, 0:cw] = g[side * half : (side + 1) * half]
                part[s, side, :, cw : 2 * cw] = u[side * half : (side + 1) * half]

        for side in (0, 1):
            c = s - SKEW * depth[side]

            @pl.when(jnp.logical_and(within(c), depth[side] == 0))
            def _():
                csend[side, c] = part[c, side].astype(BF16)
                chain_copy(side, c).start()

            @pl.when(jnp.logical_and(within(c), jnp.logical_and(depth[side] > 0, depth[side] < last)))
            def _():
                chain_copy(side, c).wait_recv()
                csend[side, c] = (part[c, side] + crecv[side, c].astype(F32)).astype(BF16)
                chain_copy(side, c).start()

            @pl.when(jnp.logical_and(within(c), depth[side] == last))
            def _():
                @pl.when(c == 0)
                def _():
                    squares = msq_send[side]
                    for d in range(1, kv):
                        sender = d if side == 0 else last - d
                        squares_copy(side, sender).wait_recv()
                        squares = squares + msq_recv[sender]
                    inv_ref[...] = lax.rsqrt(squares / model_width + EPS)

                chain_copy(side, c).wait_recv()
                both = (part[c, side] + crecv[side, c].astype(F32)) * inv_ref[:, 0:1]
                g = both[:, 0:cw]
                h_all[side, c] = (g / (1.0 + jnp.exp(-g)) * both[:, cw : 2 * cw]).astype(BF16)
                hidden_copy(side, c).start()

        for side in (0, 1):
            behind = depth[1 - side]
            c = s - full - SKEW * behind

            @pl.when(jnp.logical_and(within(c), behind > 0))
            def _():
                hidden_copy(side, c).wait_recv()

                @pl.when(behind < last)
                def _():
                    hidden_copy(side, c).start()

        c = s - full - SKEW * jnp.maximum(depth[0], depth[1])

        @pl.when(within(c))
        def _():
            lhs = jnp.concatenate([h_all[0, c].astype(F32), h_all[1, c].astype(F32)], axis=0)
            acc[...] += dot(lhs.astype(BF16), wd[pl.ds(pl.multiple_of(c * cw, cw), cw), :])

        return carry

    lax.fori_loop(0, chunks + 2 * full, step, 0)
    cut(acc[...], dsend, dt, tp)
    sends += start_all("tp", tp, t, lambda k: dsend.at[k], drecv, d_s, d_r)
    drecv[t] = dsend[t]
    wait_all("tp", tp, t, drecv, d_s, d_r)
    total = drecv[0].astype(F32)
    for j in range(1, tp):
        total = total + drecv[j].astype(F32)
    result[...] = (mid_all[t].astype(F32) + total).astype(BF16)
    for copy in sends:
        copy.wait_send()
    for side in (0, 1):
        @pl.when(jnp.logical_not(places[side]))
        def _():
            squares_copy(side, z).wait_send()

    def drain(c, carry):
        for side in (0, 1):
            @pl.when(depth[side] < last)
            def _():
                chain_copy(side, c).wait_send()

            @pl.when(depth[1 - side] < last)
            def _():
                hidden_copy(side, c).wait_send()
        return carry

    lax.fori_loop(0, chunks, drain, 0)


def state_kernel(memory_h, keys, values, out_h, held, made, in_sem, out_sem):
    own, heads, head, _ = held.shape
    first = lax.axis_index("tp") * heads
    reads = [pltpu.make_async_copy(memory_h.at[b], held.at[b], in_sem.at[b]) for b in range(own)]
    writes = [pltpu.make_async_copy(made.at[b], out_h.at[b], out_sem.at[b]) for b in range(own)]
    for copy in reads:
        copy.start()
    for b in range(own):
        reads[b].wait()
        for h in range(heads):
            exponent = -5.0 - (first + h).astype(F32) * (7.0 / max(HEADS - 1, 1))
            decay = 1.0 - jnp.exp2(jnp.full((1, head), exponent, F32))
            row = values[b : b + 1, h * head : (h + 1) * head]
            made[b, h] = decay * held[b, h] + keys[h, :, b : b + 1] * row
        writes[b].start()
    for copy in writes:
        copy.wait()


def per_device(kv, tp, tokens, lengths, memory, norm_attn, w_query, w_key, w_value, w_gate,
               head_gain, w_out, norm_mlp, w_gate_mlp, w_up, w_down):
    own, heads, head, _ = memory.shape
    rows, dt = tokens.shape
    dk, wl = w_query.shape
    ff = w_up.shape[1]
    cw = chunk_width(ff)
    chunks = ff // cw
    half = head // 2
    inverse = 10000.0 ** (-jnp.arange(half, dtype=F32) / half)
    inverse = jnp.concatenate([inverse, inverse])
    angles = lengths.astype(F32)[:, None] * inverse[None, :]
    sign = jnp.where(jnp.arange(head) < half, -1.0, 1.0)[None, :]
    vm = pl.BlockSpec(memory_space=pltpu.VMEM)
    hbm = pl.BlockSpec(memory_space=pl.ANY)
    dma = pltpu.SemaphoreType.DMA
    padded = -(-own // 8) * 8

    def pair(n, *lead):
        return [dma(lead + (n - 1,)), dma(lead + (n,))]

    scratch = [
        pltpu.VMEM(memory.shape, F32),
        *[pltpu.VMEM((dk, wl), BF16)] * 4,
        pltpu.VMEM((wl, dk), BF16),
        pltpu.VMEM((dk, ff), BF16),
        pltpu.VMEM((dk, ff), BF16),
        pltpu.VMEM((ff, dk), BF16),
        pltpu.VMEM((tp, rows, dt), BF16),
        pltpu.VMEM((rows, wl), F32),
        pltpu.VMEM((4, kv, own, wl), BF16),
        pltpu.VMEM((4, kv, own, wl), BF16),
        pltpu.VMEM((kv, own, 128), F32),
        pltpu.VMEM((kv, own, 128), F32),
        pltpu.VMEM((heads, padded, head), F32),
        pltpu.VMEM((heads, own, head), F32),
        pltpu.VMEM((heads, own, head), F32),
        pltpu.VMEM((kv, own, wl), BF16),
        pltpu.VMEM((rows, wl), F32),
        pltpu.VMEM((tp, rows, dt), BF16),
        pltpu.VMEM((tp, rows, dt), BF16),
        pltpu.VMEM((tp, rows, dt), BF16),
        pltpu.VMEM((2, rows // 2, 128), F32),
        pltpu.VMEM((kv, rows // 2, 128), F32),
        pltpu.VMEM((rows // 2, 128), F32),
        pltpu.VMEM((rows, dk), BF16),
        pltpu.VMEM((chunks, 2, rows // 2, 2 * cw), F32),
        pltpu.VMEM((2, chunks, rows // 2, 2 * cw), BF16),
        pltpu.VMEM((2, chunks, rows // 2, 2 * cw), BF16),
        pltpu.VMEM((2, chunks, rows // 2, cw), BF16),
        pltpu.VMEM((rows, dk), F32),
        pltpu.VMEM((tp, rows, dt), BF16),
        pltpu.VMEM((tp, rows, dt), BF16),
        dma((9,)),
        *pair(tp), *pair(kv), *pair(kv, 4), *pair(kv), *pair(tp), *pair(tp), *pair(tp),
        dma((2,)), dma((kv,)), *[dma((2, chunks))] * 4,
    ]
    result, keys, values = pl.pallas_call(
        functools.partial(kernel, kv, tp, float(dk * kv)),
        out_shape=(
            jax.ShapeDtypeStruct((rows, dt), BF16),
            jax.ShapeDtypeStruct((heads, head, padded), F32),
            jax.ShapeDtypeStruct((own, wl), F32),
        ),
        in_specs=[vm] * 6 + [hbm] * 9,
        out_specs=(vm, vm, vm),
        scratch_shapes=scratch,
        compiler_params=pltpu.CompilerParams(
            collective_id=0, has_side_effects=True, vmem_limit_bytes=60 * 1024 * 1024
        ),
    )(
        tokens, jnp.cos(angles), jnp.sin(angles) * sign,
        norm_attn.reshape(-1, 128), norm_mlp.reshape(-1, 128), head_gain.reshape(-1, 128),
        memory, w_query, w_key, w_value, w_gate, w_out, w_gate_mlp, w_up, w_down,
    )
    new_memory = pl.pallas_call(
        state_kernel,
        out_shape=jax.ShapeDtypeStruct(memory.shape, F32),
        in_specs=[hbm, vm, vm],
        out_specs=hbm,
        scratch_shapes=[pltpu.VMEM(memory.shape, F32), pltpu.VMEM(memory.shape, F32), dma((own,)), dma((own,))],
        compiler_params=pltpu.CompilerParams(vmem_limit_bytes=40 * 1024 * 1024),
    )(memory, keys, values)
    return result, new_memory


def solution(mesh):
    in_specs = (
        P("grp", ("kv", "tp")),
        P(("grp", "kv")),
        P(("grp", "kv"), "tp", None, None),
        P("kv"),
        P("kv", "tp"),
        P("kv", "tp"),
        P("kv", "tp"),
        P("kv", "tp"),
        P("tp"),
        P("tp", "kv"),
        P("kv"),
        P("kv", "tp"),
        P("kv", "tp"),
        P("tp", "kv"),
    )
    out_specs = (P("grp", ("kv", "tp")), P(("grp", "kv"), "tp", None, None))
    return jax.shard_map(
        functools.partial(per_device, mesh.shape["kv"], mesh.shape["tp"]),
        mesh=mesh, in_specs=in_specs, out_specs=out_specs, check_vma=False,
    )
```

```python
import functools

import jax
import jax.numpy as jnp
from jax import lax
from jax.experimental import pallas as pl
from jax.experimental.pallas import tpu as pltpu
from jax.sharding import PartitionSpec as P

HEADS = 16
EPS = 1e-06
F32 = jnp.float32
BF16 = jnp.bfloat16
MESH = pl.DeviceIdType.MESH


def dot(a, b):
    return jnp.dot(a, b, preferred_element_type=F32)


def chunk_width(ff_local):
    return 512 if ff_local % 512 == 0 else 128


SKEW = 2


def as_row(ref):
    parts = ref[...].astype(F32)
    return jnp.concatenate([parts[i : i + 1] for i in range(parts.shape[0])], axis=1)


def start_all(axis, n, me, src_of, dst, ssem, rsem):
    copies = []
    for d in range(1, n):
        other = lax.rem(me + d, n)
        copy = pltpu.make_async_remote_copy(
            src_ref=src_of(other),
            dst_ref=dst.at[me],
            send_sem=ssem.at[d - 1],
            recv_sem=rsem.at[me],
            device_id={axis: other},
            device_id_type=MESH,
        )
        copy.start()
        copies.append(copy)
    return copies


def wait_all(axis, n, me, dst, ssem, rsem):
    for d in range(1, n):
        other = lax.rem(me + d, n)
        pltpu.make_async_remote_copy(
            src_ref=dst.at[other],
            dst_ref=dst.at[other],
            send_sem=ssem.at[d - 1],
            recv_sem=rsem.at[other],
            device_id={axis: other},
            device_id_type=MESH,
        ).wait_recv()


def spread(width, total, start):
    rows = lax.broadcasted_iota(jnp.int32, (width, total), 0)
    cols = lax.broadcasted_iota(jnp.int32, (width, total), 1)
    return jnp.where(rows + start == cols, 1.0, 0.0).astype(BF16)


def pick(width, total, start):
    rows = lax.broadcasted_iota(jnp.int32, (total, width), 0)
    cols = lax.broadcasted_iota(jnp.int32, (total, width), 1)
    return jnp.where(rows == cols + start, 1.0, 0.0).astype(BF16)


def joined(blocks, dt, tp):
    if dt % 128 == 0:
        return jnp.concatenate([blocks[j].astype(F32) for j in range(tp)], axis=1)
    total = dot(blocks[0], spread(dt, dt * tp, 0))
    for j in range(1, tp):
        total = total + dot(blocks[j], spread(dt, dt * tp, j * dt))
    return total


def cut(part, buffer, dt, tp):
    if dt % 128 == 0:
        for j in range(tp):
            buffer[j] = part[:, j * dt : (j + 1) * dt].astype(BF16)
    else:
        whole = part.astype(BF16)
        for j in range(tp):
            buffer[j] = dot(whole, pick(dt, dt * tp, j * dt)).astype(BF16)


def kernel(
    kv, tp, model_width,
    tokens, cosine, sine, norm_attn, norm_mlp, gain_h,
    memory_h, wq_h, wk_h, wv_h, wg_h, wo_h, wgm_h, wup_h, wd_h,
    result, k_out, v_out,
    memory, wq, wk, wv, wg, wo, wgm, wup, wd,
    tok_all, p32, psend, precv, sq_send, sq_recv, qpad, qrot, ro, mixed_all, m32,
    asend, arecv, mid_all, msq_send, msq_recv, inv_ref, scaled_ref,
    part, csend, crecv, h_all, acc, dsend, drecv,
    lsem, tok_s, tok_r, sq_s, sq_r, p_s, p_r, mx_s, mx_r, a_s, a_r, md_s, md_r, d_s, d_r,
    ms_s, ms_r, c_s, c_r, h_s, h_r,
):
    z = lax.axis_index("kv")
    t = lax.axis_index("tp")
    rows, dt = tokens.shape
    own, heads, head, _ = memory.shape
    wl = heads * head
    ff = wup.shape[1]
    cw = chunk_width(ff)
    chunks = ff // cw

    local = []
    for i, (src, dst) in enumerate(
        [(wq_h, wq), (wk_h, wk), (wv_h, wv), (wg_h, wg), (memory_h, memory),
         (wo_h, wo), (wgm_h, wgm), (wup_h, wup), (wd_h, wd)]
    ):
        copy = pltpu.make_async_copy(src, dst, lsem.at[i])
        copy.start()
        local.append(copy)

    barrier = pltpu.get_barrier_semaphore()
    for d in range(1, kv):
        pl.semaphore_signal(barrier, inc=1, device_id={"kv": lax.rem(z + d, kv)}, device_id_type=MESH)
    for d in range(1, tp):
        pl.semaphore_signal(barrier, inc=1, device_id={"tp": lax.rem(t + d, tp)}, device_id_type=MESH)
    pl.semaphore_wait(barrier, kv + tp - 2)

    sends = []
    sends += start_all("tp", tp, t, lambda k: tokens, tok_all, tok_s, tok_r)
    tok_all[t] = tokens[...]
    wait_all("tp", tp, t, tok_all, tok_s, tok_r)
    tok = joined(tok_all, dt, tp)
    scaled = (tok * as_row(norm_attn)).astype(BF16)
    m32[:, 0:128] = jnp.broadcast_to(jnp.sum(tok * tok, axis=1, keepdims=True), (rows, 128))
    for k in range(kv):
        sq_send[k] = m32[k * own : (k + 1) * own, 0:128]
    sends += start_all("kv", kv, z, lambda k: sq_send.at[k], sq_recv, sq_s, sq_r)
    sq_recv[z] = sq_send[z]

    for i, w in enumerate((wq, wk, wv, wg)):
        local[i].wait()
        p32[...] = dot(scaled, w[...])
        for k in range(kv):
            psend[i, k] = p32[k * own : (k + 1) * own, :].astype(BF16)
        sends += start_all("kv", kv, z, lambda k: psend.at[i, k], precv.at[i], p_s.at[i], p_r.at[i])
        precv[i, z] = psend[i, z]
    qpad[...] = jnp.zeros(qpad.shape, F32)
    wait_all("kv", kv, z, sq_recv, sq_s, sq_r)
    squares = sq_recv[0]
    for k in range(1, kv):
        squares = squares + sq_recv[k]
    inv = lax.rsqrt(squares / model_width + EPS)

    def column(i, h):
        start = h * head
        total = precv[i, 0, :, start : start + head].astype(F32)
        for k in range(1, kv):
            total = total + precv[i, k, :, start : start + head].astype(F32)
        return total * inv

    cos = cosine[...]
    sin = sine[...]
    gain = as_row(gain_h)
    local[4].wait()
    wait_all("kv", kv, z, precv.at[0], p_s.at[0], p_r.at[0])
    for h in range(heads):
        q = column(0, h)
        q = (q * cos + pltpu.roll(q, head // 2, 1) * sin) * head ** (-0.5)
        qrot[h] = q
        qpad[h, 0:own, :] = q
        q_t = jnp.transpose(qpad[h])
        for b in range(own):
            ro[h, b : b + 1, :] = jnp.sum(memory[b, h] * q_t[:, b : b + 1], axis=0, keepdims=True)
    for i in (1, 2, 3):
        wait_all("kv", kv, z, precv.at[i], p_s.at[i], p_r.at[i])
    for h in range(heads):
        kk = column(1, h)
        kk = kk * cos + pltpu.roll(kk, head // 2, 1) * sin
        v = column(2, h)
        g = column(3, h)
        qpad[h, 0:own, :] = kk
        v_out[:, h * head : (h + 1) * head] = v
        exponent = -5.0 - (t * heads + h).astype(F32) * (7.0 / max(HEADS - 1, 1))
        decay = 1.0 - jnp.exp2(jnp.full((1, head), exponent, F32))
        readout = decay * ro[h] + jnp.sum(qrot[h] * kk, axis=1, keepdims=True) * v
        centred = readout - jnp.mean(readout, axis=1, keepdims=True)
        normed = centred * lax.rsqrt(jnp.mean(centred * centred, axis=1, keepdims=True) + EPS)
        mixed = normed * gain[:, h * head : (h + 1) * head] * (g / (1.0 + jnp.exp(-g)))
        mixed_all[z, :, h * head : (h + 1) * head] = mixed.astype(BF16)

    sends += start_all("kv", kv, z, lambda k: mixed_all.at[z], mixed_all, mx_s, mx_r)
    for h in range(heads):
        k_out[h] = jnp.transpose(qpad[h])
    local[5].wait()
    wait_all("kv", kv, z, mixed_all, mx_s, mx_r)
    for k in range(kv):
        m32[k * own : (k + 1) * own, :] = mixed_all[k].astype(F32)
    cut(dot(m32[...].astype(BF16), wo[...]), asend, dt, tp)
    sends += start_all("tp", tp, t, lambda k: asend.at[k], arecv, a_s, a_r)
    arecv[t] = asend[t]
    wait_all("tp", tp, t, arecv, a_s, a_r)
    total = arecv[0].astype(F32)
    for j in range(1, tp):
        total = total + arecv[j].astype(F32)
    mid_all[t] = (tokens[...].astype(F32) + total).astype(BF16)
    sends += start_all("tp", tp, t, lambda k: mid_all.at[t], mid_all, md_s, md_r)
    local[6].wait()
    local[7].wait()
    wait_all("tp", tp, t, mid_all, md_s, md_r)
    mid = joined(mid_all, dt, tp)
    scaled = (mid * as_row(norm_mlp)).astype(BF16)
    scaled_ref[...] = scaled
    mid_squares = jnp.broadcast_to(jnp.sum(mid * mid, axis=1, keepdims=True), (rows, 128))
    half = rows // 2
    last = kv - 1
    places = (z == 0, z == last)
    ends = (0, last)
    for side in (0, 1):
        msq_send[side] = mid_squares[side * half : (side + 1) * half]

    def squares_copy(side, sender):
        return pltpu.make_async_remote_copy(
            src_ref=msq_send.at[side],
            dst_ref=msq_recv.at[sender],
            send_sem=ms_s.at[side],
            recv_sem=ms_r.at[sender],
            device_id={"kv": ends[side]},
            device_id_type=MESH,
        )

    for side in (0, 1):
        @pl.when(jnp.logical_not(places[side]))
        def _():
            squares_copy(side, z).start()

    onward = (lax.rem(z + last, kv), lax.rem(z + 1, kv))
    depth = (last - z, z)

    def chain_copy(side, c):
        return pltpu.make_async_remote_copy(
            src_ref=csend.at[side, c],
            dst_ref=crecv.at[side, c],
            send_sem=c_s.at[side, c],
            recv_sem=c_r.at[side, c],
            device_id={"kv": onward[side]},
            device_id_type=MESH,
        )

    def hidden_copy(side, c):
        return pltpu.make_async_remote_copy(
            src_ref=h_all.at[side, c],
            dst_ref=h_all.at[side, c],
            send_sem=h_s.at[side, c],
            recv_sem=h_r.at[side, c],
            device_id={"kv": onward[1 - side]},
            device_id_type=MESH,
        )

    def within(c):
        return jnp.logical_and(c >= 0, c < chunks)

    acc[...] = jnp.zeros(acc.shape, F32)
    local[8].wait()
    full = SKEW * last

    def step(s, carry):
        @pl.when(s < chunks)
        def _():
            cols = pl.ds(pl.multiple_of(s * cw, cw), cw)
            lhs = scaled_ref[...]
            g = dot(lhs, wgm[:, cols])
            u = dot(lhs, wup[:, cols])
            for side in (0, 1):
                part[s, side, :, 0:cw] = g[side * half : (side + 1) * half]
                part[s, side, :, cw : 2 * cw] = u[side * half : (side + 1) * half]

        for side in (0, 1):
            c = s - SKEW * depth[side]

            @pl.when(jnp.logical_and(within(c), depth[side] == 0))
            def _():
                csend[side, c] = part[c, side].astype(BF16)
                chain_copy(side, c).start()

            @pl.when(jnp.logical_and(within(c), jnp.logical_and(depth[side] > 0, depth[side] < last)))
            def _():
                chain_copy(side, c).wait_recv()
                csend[side, c] = (part[c, side] + crecv[side, c].astype(F32)).astype(BF16)
                chain_copy(side, c).start()

            @pl.when(jnp.logical_and(within(c), depth[side] == last))
            def _():
                @pl.when(c == 0)
                def _():
                    squares = msq_send[side]
                    for d in range(1, kv):
                        sender = d if side == 0 else last - d
                        squares_copy(side, sender).wait_recv()
                        squares = squares + msq_recv[sender]
                    inv_ref[...] = lax.rsqrt(squares / model_width + EPS)

                chain_copy(side, c).wait_recv()
                both = (part[c, side] + crecv[side, c].astype(F32)) * inv_ref[:, 0:1]
                g = both[:, 0:cw]
                h_all[side, c] = (g / (1.0 + jnp.exp(-g)) * both[:, cw : 2 * cw]).astype(BF16)
                hidden_copy(side, c).start()

        for side in (0, 1):
            behind = depth[1 - side]
            c = s - full - SKEW * behind

            @pl.when(jnp.logical_and(within(c), behind > 0))
            def _():
                hidden_copy(side, c).wait_recv()

                @pl.when(behind < last)
                def _():
                    hidden_copy(side, c).start()

        c = s - full - SKEW * jnp.maximum(depth[0], depth[1])

        @pl.when(within(c))
        def _():
            lhs = jnp.concatenate([h_all[0, c].astype(F32), h_all[1, c].astype(F32)], axis=0)
            acc[...] += dot(lhs.astype(BF16), wd[pl.ds(pl.multiple_of(c * cw, cw), cw), :])

        return carry

    lax.fori_loop(0, chunks + 2 * full, step, 0)
    cut(acc[...], dsend, dt, tp)
    sends += start_all("tp", tp, t, lambda k: dsend.at[k], drecv, d_s, d_r)
    drecv[t] = dsend[t]
    wait_all("tp", tp, t, drecv, d_s, d_r)
    total = drecv[0].astype(F32)
    for j in range(1, tp):
        total = total + drecv[j].astype(F32)
    result[...] = (mid_all[t].astype(F32) + total).astype(BF16)
    for copy in sends:
        copy.wait_send()
    for side in (0, 1):
        @pl.when(jnp.logical_not(places[side]))
        def _():
            squares_copy(side, z).wait_send()

    def drain(c, carry):
        for side in (0, 1):
            @pl.when(depth[side] < last)
            def _():
                chain_copy(side, c).wait_send()

            @pl.when(depth[1 - side] < last)
            def _():
                hidden_copy(side, c).wait_send()
        return carry

    lax.fori_loop(0, chunks, drain, 0)


def state_kernel(memory_h, keys_h, values_h, out_h, held, made, keys, values, in_sem, out_sem, kv_sem):
    own, heads, head, _ = held.shape
    first = lax.axis_index("tp") * heads
    reads = [pltpu.make_async_copy(memory_h.at[b], held.at[b], in_sem.at[b]) for b in range(own)]
    writes = [pltpu.make_async_copy(made.at[b], out_h.at[b], out_sem.at[b]) for b in range(own)]
    rows = [pltpu.make_async_copy(keys_h, keys, kv_sem.at[0]), pltpu.make_async_copy(values_h, values, kv_sem.at[1])]
    for copy in rows + reads:
        copy.start()
    decays = []
    for h in range(heads):
        exponent = -5.0 - (first + h).astype(F32) * (7.0 / max(HEADS - 1, 1))
        decays.append(1.0 - jnp.exp2(jnp.full((1, head), exponent, F32)))
    for copy in rows:
        copy.wait()
    for b in range(own):
        reads[b].wait()
        for h in range(heads):
            row = values[b : b + 1, h * head : (h + 1) * head]
            made[b, h] = decays[h] * held[b, h] + keys[h, :, b : b + 1] * row
        writes[b].start()
    for copy in writes:
        copy.wait()


def per_device(kv, tp, tokens, lengths, memory, norm_attn, w_query, w_key, w_value, w_gate,
               head_gain, w_out, norm_mlp, w_gate_mlp, w_up, w_down):
    own, heads, head, _ = memory.shape
    rows, dt = tokens.shape
    dk, wl = w_query.shape
    ff = w_up.shape[1]
    cw = chunk_width(ff)
    chunks = ff // cw
    half = head // 2
    inverse = 10000.0 ** (-jnp.arange(half, dtype=F32) / half)
    inverse = jnp.concatenate([inverse, inverse])
    angles = lengths.astype(F32)[:, None] * inverse[None, :]
    sign = jnp.where(jnp.arange(head) < half, -1.0, 1.0)[None, :]
    vm = pl.BlockSpec(memory_space=pltpu.VMEM)
    hbm = pl.BlockSpec(memory_space=pl.ANY)
    dma = pltpu.SemaphoreType.DMA
    padded = -(-own // 8) * 8

    def pair(n, *lead):
        return [dma(lead + (n - 1,)), dma(lead + (n,))]

    scratch = [
        pltpu.VMEM(memory.shape, F32),
        *[pltpu.VMEM((dk, wl), BF16)] * 4,
        pltpu.VMEM((wl, dk), BF16),
        pltpu.VMEM((dk, ff), BF16),
        pltpu.VMEM((dk, ff), BF16),
        pltpu.VMEM((ff, dk), BF16),
        pltpu.VMEM((tp, rows, dt), BF16),
        pltpu.VMEM((rows, wl), F32),
        pltpu.VMEM((4, kv, own, wl), BF16),
        pltpu.VMEM((4, kv, own, wl), BF16),
        pltpu.VMEM((kv, own, 128), F32),
        pltpu.VMEM((kv, own, 128), F32),
        pltpu.VMEM((heads, padded, head), F32),
        pltpu.VMEM((heads, own, head), F32),
        pltpu.VMEM((heads, own, head), F32),
        pltpu.VMEM((kv, own, wl), BF16),
        pltpu.VMEM((rows, wl), F32),
        pltpu.VMEM((tp, rows, dt), BF16),
        pltpu.VMEM((tp, rows, dt), BF16),
        pltpu.VMEM((tp, rows, dt), BF16),
        pltpu.VMEM((2, rows // 2, 128), F32),
        pltpu.VMEM((kv, rows // 2, 128), F32),
        pltpu.VMEM((rows // 2, 128), F32),
        pltpu.VMEM((rows, dk), BF16),
        pltpu.VMEM((chunks, 2, rows // 2, 2 * cw), F32),
        pltpu.VMEM((2, chunks, rows // 2, 2 * cw), BF16),
        pltpu.VMEM((2, chunks, rows // 2, 2 * cw), BF16),
        pltpu.VMEM((2, chunks, rows // 2, cw), BF16),
        pltpu.VMEM((rows, dk), F32),
        pltpu.VMEM((tp, rows, dt), BF16),
        pltpu.VMEM((tp, rows, dt), BF16),
        dma((9,)),
        *pair(tp), *pair(kv), *pair(kv, 4), *pair(kv), *pair(tp), *pair(tp), *pair(tp),
        dma((2,)), dma((kv,)), *[dma((2, chunks))] * 4,
    ]
    result, keys, values = pl.pallas_call(
        functools.partial(kernel, kv, tp, float(dk * kv)),
        out_shape=(
            jax.ShapeDtypeStruct((rows, dt), BF16),
            jax.ShapeDtypeStruct((heads, head, padded), F32),
            jax.ShapeDtypeStruct((own, wl), F32),
        ),
        in_specs=[vm] * 6 + [hbm] * 9,
        out_specs=(vm, vm, vm),
        scratch_shapes=scratch,
        compiler_params=pltpu.CompilerParams(
            collective_id=0, has_side_effects=True, vmem_limit_bytes=60 * 1024 * 1024
        ),
    )(
        tokens, jnp.cos(angles), jnp.sin(angles) * sign,
        norm_attn.reshape(-1, 128), norm_mlp.reshape(-1, 128), head_gain.reshape(-1, 128),
        memory, w_query, w_key, w_value, w_gate, w_out, w_gate_mlp, w_up, w_down,
    )
    new_memory = pl.pallas_call(
        state_kernel,
        out_shape=jax.ShapeDtypeStruct(memory.shape, F32),
        in_specs=[hbm, hbm, hbm],
        out_specs=hbm,
        scratch_shapes=[
            pltpu.VMEM(memory.shape, F32), pltpu.VMEM(memory.shape, F32),
            pltpu.VMEM(keys.shape, F32), pltpu.VMEM(values.shape, F32),
            dma((own,)), dma((own,)), dma((2,)),
        ],
        compiler_params=pltpu.CompilerParams(vmem_limit_bytes=63 * 1024 * 1024),
    )(memory, keys, values)
    return result, new_memory


def solution(mesh):
    in_specs = (
        P("grp", ("kv", "tp")),
        P(("grp", "kv")),
        P(("grp", "kv"), "tp", None, None),
        P("kv"),
        P("kv", "tp"),
        P("kv", "tp"),
        P("kv", "tp"),
        P("kv", "tp"),
        P("tp"),
        P("tp", "kv"),
        P("kv"),
        P("kv", "tp"),
        P("kv", "tp"),
        P("tp", "kv"),
    )
    out_specs = (P("grp", ("kv", "tp")), P(("grp", "kv"), "tp", None, None))
    return jax.shard_map(
        functools.partial(per_device, mesh.shape["kv"], mesh.shape["tp"]),
        mesh=mesh, in_specs=in_specs, out_specs=out_specs, check_vma=False,
    )
```
